32 devices in a mesh: sp: 8 (over z, y), tp: 4 (over x, core).
Axes of the slice: x: 2, y: 2, z: 4, core: 2. Of those that a mesh axis runs over, the one named last changes fastest.
Arguments:
- tokens: bfloat16 [8192, 2048], P('sp', 'tp'), may hold values from -600 to 600, as said below
- norm_gain: float32 [2048], replicated, may hold values from 0.1 to 1.9
- w_query: bfloat16 [2048, 1024], P(None, 'tp'), may hold values from -0.125 to 0.125
- w_forget_fwd: bfloat16 [2048, 1024], P(None, 'tp'), may hold values from -0.125 to 0.125
- w_forget_bwd: bfloat16 [2048, 1024], P(None, 'tp'), may hold values from -0.125 to 0.125
- w_value: bfloat16 [2048, 1024], P(None, 'tp'), may hold values from -0.125 to 0.125
- w_gate: bfloat16 [2048, 1024], P(None, 'tp'), may hold values from -0.125 to 0.125
- w_pool_in: bfloat16 [2048, 1024], P(None, 'tp'), may hold values from -0.125 to 0.125
- forget_gap: float32 [2, 1024], P(None, 'tp'), may hold values from 0 to 0.06
- added_log_retention: float32 [8192, 8], P('sp', 'tp'), may hold values from -2.1 to 0
- initial_state: float32 [2, 8, 128, 128], P(None, 'tp'), may hold values from -0.18 to 0.18
- head_gain: float32 [1024], P('tp'), may hold values from 0.1 to 1.9
- pool_mix: bfloat16 [4, 256, 256], P('tp'), may hold values from -0.375 to 0.375
- pool_gain: float32 [1024], P('tp'), may hold values from 0.1 to 1.9
- w_out_recur: bfloat16 [1024, 2048], P('tp'), may hold values from -0.125 to 0.125
- w_out_pool: bfloat16 [1024, 2048], P('tp'), may hold values from -0.125 to 0.125
Outputs:
- mixed_out: bfloat16 [8192, 2048], P(('sp', 'tp'))
The draws below stay inside these ranges and needn't reach their ends.
Inputs may be any that keep to these rules, and one draw needn't show every extreme that they name: `tokens`: layer input with scales that differ between rows and between columns.
All inputs are finite; a program needn't handle non-finite values.
Results may differ from the reference program's by a relative error of at most 0.013.
Values may be sent and summed in bfloat16 or wider, within the bound.
A program may use at most 128 MiB of HBM per device.

```python
import jax
import jax.numpy as jnp
from jax import lax

D = 2048
HEADS = 8
HEAD_DIM = 128
EXPAND = 128
POOL_GROUPS = 4
POOL_GROUP = 256
BLOCK = 64
TOK_DEV = 1024
SEQ = 8192
HG_WIDTH = 1024
KDIM = 1024
POOL_WIDTH = 1024
N_TP = 4


def draw_tokens(key, part):
    first, second, third = jax.random.split(key, 3)
    base = jnp.clip(jax.random.normal(first, (SEQ, D), jnp.float32), -6.0, 6.0)
    row_scale = 10.0 ** jax.random.uniform(second, (SEQ, 1), jnp.float32, 0.0, 1.0)
    rising = jnp.arange(D, dtype=jnp.float32) / D
    column_scale = 10.0 ** (0.8 * rising + jax.random.uniform(third, (1, D), jnp.float32, 0.0, 0.2))
    return (base * row_scale * column_scale).astype(jnp.bfloat16)


def draw_forget_gap(key, part):
    pick_key, fast_key, slow_key = jax.random.split(key, 3)
    share = 0.5
    fast_heads = jax.random.uniform(pick_key, (2, HEADS, 1), jnp.float32) < share
    fast_gap = jax.random.uniform(fast_key, (2, HEADS, EXPAND), jnp.float32, 0.02, 0.06)
    lowest = jnp.log(jnp.float32(0.3 / SEQ))
    highest = jnp.log(jnp.float32(min(30.0 / SEQ, 0.06)))
    slow_gap = jnp.exp(jax.random.uniform(slow_key, (2, HEADS, EXPAND), jnp.float32, lowest, highest))
    return jnp.where(fast_heads, fast_gap, slow_gap).reshape(2, HEADS * EXPAND)


def draw_added_log_retention(key, part):
    level_key, where_key, size_key = jax.random.split(key, 3)
    span = max(TOK_DEV // 4, 1)
    pieces = SEQ // span
    lowest = jnp.log(jnp.float32(0.1 / SEQ))
    highest = jnp.log(jnp.float32(1.0 / SEQ))
    level = jnp.exp(jax.random.uniform(level_key, (pieces, 1, HEADS), jnp.float32, lowest, highest))
    backdrop_term = -jnp.broadcast_to(level, (pieces, span, HEADS)).reshape(SEQ, HEADS)
    spots = jax.random.randint(where_key, (3, HEADS), 0, SEQ)
    layer_depth = jax.random.uniform(size_key, (3, HEADS), jnp.float32, 0.22, 0.69)
    location_list = jnp.arange(SEQ, dtype=jnp.int32)[:, None, None] == spots[None, :, :]
    token_groups = -jnp.sum(jnp.where(location_list, layer_depth[None, :, :], 0.0), axis=1)
    return backdrop_term + token_groups


def steps_of(rng, shape, cuts, low, largest):
    loudness = 1.0
    for dim, parts in cuts:
        heights = jax.random.uniform(jax.random.fold_in(jax.random.fold_in(rng, 6), dim), (parts,), jnp.float32, low / len(cuts), largest / len(cuts))
        loudness = loudness * jnp.repeat(jnp.exp(heights), shape[dim] // parts).reshape((-1,) + (1,) * (len(shape) - 1 - dim))
    return loudness


def normal_values(rng, dims, deviation, most, shards=(), kind=jnp.bfloat16):
    factor_of = steps_of(rng, dims, shards, -0.22, 0.18) if shards else 1.0
    values = jax.random.normal(rng, dims, jnp.float32) * deviation * factor_of
    return jnp.minimum(jnp.maximum(values, -most), most).astype(kind)


def setup_inputs(seed: int = 0) -> dict:
    streams_of = jax.random.split(jax.random.key(seed), 17)
    return {
        "tokens": draw_tokens(jax.random.fold_in(streams_of[16], 71), 0),
        "norm_gain": jnp.clip(1.0 + 0.18 * jax.random.normal(streams_of[1], (D,), jnp.float32), 0.1, 1.9),
        "w_query": normal_values(streams_of[2], (D, KDIM), D ** -0.5, 0.125, ((1, 4),)),
        "w_forget_fwd": normal_values(streams_of[3], (D, KDIM), D ** -0.5, 0.125, ((1, 4),)),
        "w_forget_bwd": normal_values(streams_of[4], (D, KDIM), D ** -0.5, 0.125, ((1, 4),)),
        "w_value": normal_values(streams_of[5], (D, HG_WIDTH), D ** -0.5, 0.125, ((1, 4),)),
        "w_gate": normal_values(streams_of[6], (D, HG_WIDTH), D ** -0.5, 0.125, ((1, 4),)),
        "w_pool_in": normal_values(streams_of[7], (D, POOL_WIDTH), D ** -0.5, 0.125, ((1, 4),)),
        "forget_gap": draw_forget_gap(jax.random.fold_in(streams_of[16], 71), 0),
        "added_log_retention": draw_added_log_retention(jax.random.fold_in(streams_of[16], 71), 0),
        "initial_state": normal_values(streams_of[10], (2, HEADS, EXPAND, HEAD_DIM), 0.03, 0.18, ((1, 4),), jnp.float32),
        "head_gain": jnp.clip(1.0 + 0.18 * jax.random.normal(streams_of[11], (HG_WIDTH,), jnp.float32), 0.1, 1.9),
        "pool_mix": normal_values(streams_of[12], (POOL_GROUPS, POOL_GROUP, POOL_GROUP), POOL_GROUP ** -0.5, 0.375, ((0, 4),)),
        "pool_gain": jnp.clip(1.0 + 0.18 * jax.random.normal(streams_of[13], (POOL_WIDTH,), jnp.float32), 0.1, 1.9),
        "w_out_recur": normal_values(streams_of[14], (HG_WIDTH, D), (HG_WIDTH + POOL_WIDTH) ** -0.5, 0.125, ((0, 4),)),
        "w_out_pool": normal_values(streams_of[15], (POOL_WIDTH, D), (HG_WIDTH + POOL_WIDTH) ** -0.5, 0.125, ((0, 4),)),
    }


EPSILON = 1e-06
FULL_ACCURACY = lax.Precision.HIGHEST

def project(normed, scale, weight):
    return (jnp.dot(normed, weight, preferred_element_type=jnp.float32) * scale).astype(jnp.bfloat16)

def recurrence(query, block_entry, values, log_keep, start):
    length, heads, layer_depth = query.shape
    count = length // BLOCK

    def split(array):
        return array.reshape(count, BLOCK, heads, array.shape[2]).transpose(0, 2, 1, 3)
    lower = jnp.tril(jnp.ones((BLOCK, BLOCK), jnp.float32))

    def advance(hidden_state, inputs):
        query_block, entry_block, value_tile_rows, keep_block = inputs
        running = jnp.cumsum(keep_block, axis=1)
        query_retention = query_block * jnp.exp(running)
        entry_decay = entry_block * jnp.exp(-running)
        scores = jnp.einsum('hck,hsk->hcs', query_retention, entry_decay, precision=FULL_ACCURACY) * lower
        final_output = jnp.einsum('hcs,hsv->hcv', scores, value_tile_rows, precision=FULL_ACCURACY)
        final_output = final_output + jnp.einsum('rbl,rlm->rbm', query_retention, hidden_state, precision=FULL_ACCURACY)
        closing_value = running[:, -1:, :]
        final_block_entry = entry_block * jnp.exp(closing_value - running)
        hidden_state = jnp.exp(closing_value[:, 0, :, None]) * hidden_state + jnp.einsum('xnw,xnz->xwz', final_block_entry, value_tile_rows, precision=FULL_ACCURACY)
        return (hidden_state, final_output)
    hidden_state, final_output = lax.scan(advance, start, (split(query), split(block_entry), split(values), split(log_keep)))
    return final_output.transpose(0, 2, 1, 3).reshape(length, heads, values.shape[2])

def reference(tokens, norm_gain, w_query, w_forget_fwd, w_forget_bwd, w_value, w_gate, w_pool_in, forget_gap, added_log_retention, initial_state, head_gain, pool_mix, pool_gain, w_out_recur, w_out_pool):
    widened = tokens.astype(jnp.float32)
    scale = lax.rsqrt(lax.optimization_barrier(jnp.mean(widened * widened, axis=1, keepdims=True)) + EPSILON)
    normed = (widened * norm_gain).astype(jnp.bfloat16)
    query_pre = project(normed, scale, w_query)
    forget_fwd = project(normed, scale, w_forget_fwd)
    forget_bwd = project(normed, scale, w_forget_bwd)
    value_proj = project(normed, scale, w_value)
    gate_pre = project(normed, scale, w_gate)
    pool_in = project(normed, scale, w_pool_in)

    def split_heads(array, width):
        return array.astype(jnp.float32).reshape(SEQ, HEADS, width)
    query = jax.nn.silu(split_heads(query_pre, EXPAND))
    values = split_heads(value_proj, HEAD_DIM)
    token_group = added_log_retention[:, :, None]

    def gates(pre, gap):
        block_entry = gap.reshape(HEADS, EXPAND) * jax.nn.sigmoid(-split_heads(pre, EXPAND))
        return (block_entry, jnp.log1p(-block_entry) + token_group)
    entry_fwd, keep_fwd = gates(forget_fwd, forget_gap[0])
    entry_bwd, keep_bwd = gates(forget_bwd, forget_gap[1])
    out_fwd = recurrence(query, entry_fwd, values, keep_fwd, initial_state[0])
    output_backward = jnp.flip(recurrence(jnp.flip(query, 0), jnp.flip(entry_bwd, 0), jnp.flip(values, 0), jnp.flip(keep_bwd, 0), initial_state[1]), 0)
    both = out_fwd + output_backward
    both = both * lax.rsqrt(lax.optimization_barrier(jnp.mean(both * both, axis=2, keepdims=True)) + EPSILON)
    recur = (both.reshape(SEQ, HG_WIDTH) * head_gain * jax.nn.sigmoid(gate_pre.astype(jnp.float32))).astype(jnp.bfloat16)
    positions = jnp.arange(SEQ, dtype=jnp.int32)
    pooled = []
    for group in range(POOL_GROUPS):
        window = 2 ** (group + 1)
        current = pool_in[:, group * POOL_GROUP:(group + 1) * POOL_GROUP].astype(jnp.float32)
        sums = jnp.concatenate([jnp.zeros((1, POOL_GROUP), jnp.float32), jnp.cumsum(current, axis=0)], axis=0)
        low = jnp.clip(positions - window // 2, 0, SEQ)
        high = jnp.clip(positions - window // 2 + window, 0, SEQ)
        window_mean = (sums[high] - sums[low]) / (high - low).astype(jnp.float32)[:, None]
        diff = (window_mean - current).astype(jnp.bfloat16)
        pooled.append(jnp.dot(diff, pool_mix[group], preferred_element_type=jnp.float32))
    pool_out = (jnp.concatenate(pooled, axis=1) * pool_gain).astype(jnp.bfloat16)
    recur_share = HG_WIDTH // N_TP
    pool_share = POOL_WIDTH // N_TP
    total = jnp.zeros((SEQ, D), jnp.float32)
    for rank in range(N_TP):
        partial_sum = jnp.dot(recur[:, rank * recur_share:(rank + 1) * recur_share], w_out_recur[rank * recur_share:(rank + 1) * recur_share], preferred_element_type=jnp.float32)
        partial_sum = partial_sum + jnp.dot(pool_out[:, rank * pool_share:(rank + 1) * pool_share], w_out_pool[rank * pool_share:(rank + 1) * pool_share], preferred_element_type=jnp.float32)
        rounded = lax.optimization_barrier(partial_sum.astype(jnp.bfloat16))
        total = total + rounded.astype(jnp.float32)
    return total.astype(jnp.bfloat16)
```

```python
import functools

import jax
import jax.numpy as jnp
from jax import lax
from jax.experimental import pallas as pl
from jax.experimental.pallas import tpu as pltpu
from jax.sharding import PartitionSpec as P

DEPTH = 128
CHUNK = 128
EPSILON = 1e-06
MESH = pl.DeviceIdType.MESH
F32 = jnp.float32
BF16 = jnp.bfloat16
VMEM_LIMIT = 60 * 1024 * 1024
ANY = pl.BlockSpec(memory_space=pl.ANY)
VM = pl.BlockSpec(memory_space=pltpu.VMEM)


def dot(a, b):
    return jnp.dot(a, b, preferred_element_type=F32)


def dot_t(a, b):
    return lax.dot_general(a, b, (((1,), (1,)), ((), ())), preferred_element_type=F32)


def t_dot(a, b, precision=None):
    return lax.dot_general(
        a, b, (((0,), (0,)), ((), ())), preferred_element_type=F32, precision=precision
    )


def peers():
    me = lax.axis_index("tp")
    sibling = me + 1 - 2 * lax.rem(me, 2)
    across = lax.rem(me + 2, 4)
    return me, sibling, across, lax.rem(sibling + 2, 4)


def greet(*devices):
    barrier = pltpu.get_barrier_semaphore()
    for device in devices:
        pl.semaphore_signal(barrier, inc=1, device_id={"tp": device}, device_id_type=MESH)
    pl.semaphore_wait(barrier, len(devices))


def project_kernel(pieces, tokens, gain, *refs):
    weights, outs = refs[:6], refs[6:12]
    held, wide, acc, square, w_sem, sib_sem, x_send, x_recv, f_send, f_recv = refs[12:]
    me, sibling, across, opposite = peers()
    length, width = tokens.shape
    rows = length // pieces
    loads = [pltpu.make_async_copy(w, wide.at[i], w_sem.at[i]) for i, w in enumerate(weights)]
    for load in loads:
        load.start()
    greet(sibling, across)

    def crossing(i):
        at = pl.ds(i * rows, rows)
        return pltpu.make_async_remote_copy(
            tokens.at[at], held.at[1, at], x_send.at[i], x_recv.at[i],
            device_id={"tp": across}, device_id_type=MESH,
        )

    def relay(i):
        at = pl.ds(i * rows, rows)
        return pltpu.make_async_remote_copy(
            held.at[1, at], held.at[2, at], f_send.at[i], f_recv.at[i],
            device_id={"tp": sibling}, device_id_type=MESH,
        )

    beside = pltpu.make_async_remote_copy(
        tokens, held.at[0], sib_sem.at[0], sib_sem.at[1],
        device_id={"tp": sibling}, device_id_type=MESH,
    )
    for i in range(pieces):
        crossing(i).start()
    beside.start()

    def part(block, owner, at, first):
        columns = pl.ds(pl.multiple_of(owner * width, width), width)
        x = block.astype(F32)
        total = jnp.sum(x * x, axis=1, keepdims=True)
        normed = (x * gain[:, columns]).astype(BF16)
        square[at, :] = total if first else square[at, :] + total
        for j in range(6):
            y = dot(normed, wide[j, columns, :])
            acc[j, at, :] = y if first else acc[j, at, :] + y

    for load in loads:
        load.wait()

    def own(i, _):
        at = pl.ds(pl.multiple_of(i * rows, rows), rows)
        part(tokens[at, :], me, at, True)
        return 0

    lax.fori_loop(0, pieces, own, 0)
    beside.wait()

    def near(i, _):
        at = pl.ds(pl.multiple_of(i * rows, rows), rows)
        part(held[0, at, :], sibling, at, False)
        return 0

    lax.fori_loop(0, pieces, near, 0)
    features = width * 4

    def far(i, _):
        at = pl.ds(pl.multiple_of(i * rows, rows), rows)
        crossing(i).wait_recv()
        relay(i).start()
        part(held[1, at, :], across, at, False)
        relay(i).wait_recv()
        part(held[2, at, :], opposite, at, False)
        scale = lax.rsqrt(square[at, :] / features + EPSILON)
        for j in range(6):
            outs[j][at, :] = (acc[j, at, :] * scale).astype(BF16)
        return 0

    lax.fori_loop(0, pieces, far, 0)
    for i in range(pieces):
        crossing(i).wait_send()
        relay(i).wait_send()


def project(tokens, gain, weights):
    length, width = tokens.shape
    depth, columns = weights[0].shape
    pieces = 4
    return pl.pallas_call(
        functools.partial(project_kernel, pieces),
        out_shape=[jax.ShapeDtypeStruct((length, columns), BF16)] * 6,
        in_specs=[VM, VM] + [ANY] * 6,
        out_specs=[VM] * 6,
        scratch_shapes=[
            pltpu.VMEM((3, length, width), BF16),
            pltpu.VMEM((6, depth, columns), BF16),
            pltpu.VMEM((6, length, columns), F32),
            pltpu.VMEM((length, 1), F32),
            pltpu.SemaphoreType.DMA((6,)),
            pltpu.SemaphoreType.DMA((2,)),
            pltpu.SemaphoreType.DMA((pieces,)),
            pltpu.SemaphoreType.DMA((pieces,)),
            pltpu.SemaphoreType.DMA((pieces,)),
            pltpu.SemaphoreType.DMA((pieces,)),
        ],
        compiler_params=pltpu.CompilerParams(
            collective_id=0, has_side_effects=True, vmem_limit_bytes=VMEM_LIMIT
        ),
        name="project",
    )(tokens, gain, *weights)


def strides():
    count = lax.axis_size("sp")
    return [1 << k for k in range(count.bit_length()) if 1 << k < count]


def partner(d, stride):
    me, count = lax.axis_index("sp"), lax.axis_size("sp")
    above, below = me + stride < count, me >= stride
    return (above, me + stride, below) if d == 0 else (below, me - stride, above)


def meet():
    barrier = pltpu.get_barrier_semaphore()
    for stride in strides():
        for d in range(2):
            exists, target, _ = partner(d, stride)

            @pl.when(exists)
            def _():
                pl.semaphore_signal(
                    barrier, inc=1, device_id={"sp": target}, device_id_type=MESH
                )

    number = jnp.int32(0)
    for stride in strides():
        for d in range(2):
            exists, _, _ = partner(d, stride)
            number = number + jnp.where(exists, 1, 0)
    pl.semaphore_wait(barrier, number)


def edge_copy(d, pool_in, edge, e_send, e_recv):
    length, rim = pool_in.shape[0], edge.shape[1]
    _, target, _ = partner(d, 1)
    begin = length - rim if d == 0 else 0
    return pltpu.make_async_remote_copy(
        pool_in.at[pl.ds(begin, rim)], edge.at[d], e_send.at[d], e_recv.at[d],
        device_id={"sp": target}, device_id_type=MESH,
    )


def edges_start(pool_in, edge, e_send, e_recv):
    for d in range(2):
        exists, _, source = partner(d, 1)

        @pl.when(exists)
        def _():
            edge_copy(d, pool_in, edge, e_send, e_recv).start()

        @pl.when(jnp.logical_not(source))
        def _():
            edge[d] = jnp.zeros(edge.shape[1:], edge.dtype)


def edges_close(pool_in, edge, e_send, e_recv):
    for d in range(2):
        exists, _, source = partner(d, 1)

        @pl.when(source)
        def _():
            edge_copy(d, pool_in, edge, e_send, e_recv).wait_recv()

        @pl.when(exists)
        def _():
            edge_copy(d, pool_in, edge, e_send, e_recv).wait_send()


def scan_copy(k, d, stride, sent, landed, p_send, p_recv):
    _, target, _ = partner(d, stride)
    return pltpu.make_async_remote_copy(
        sent.at[k, d], landed.at[k, d], p_send.at[k, d], p_recv.at[k, d],
        device_id={"sp": target}, device_id_type=MESH,
    )


def scan_start(k, state, offset, sent, landed, before, before_keep, p_send, p_recv):
    stride, heads = strides()[k], state.shape[1]
    for d in range(2):
        exists, _, _ = partner(d, stride)

        @pl.when(exists)
        def _():
            for h in range(heads):
                lanes = slice(h * DEPTH, (h + 1) * DEPTH)
                keep = jnp.exp(offset[d, :, lanes])
                sent[k, d, h, :DEPTH, :] = (keep * before[d, h] + state[d, h]).astype(BF16)
                sent[k, d, h, DEPTH:, :] = jnp.broadcast_to(
                    keep * before_keep[d, :, lanes], (16, DEPTH)
                ).astype(BF16)
            scan_copy(k, d, stride, sent, landed, p_send, p_recv).start()


def scan_close(k, state, sent, landed, before, before_keep, p_send, p_recv):
    stride, heads = strides()[k], state.shape[1]
    for d in range(2):
        exists, _, source = partner(d, stride)

        @pl.when(source)
        def _():
            scan_copy(k, d, stride, sent, landed, p_send, p_recv).wait_recv()
            for h in range(heads):
                lanes = slice(h * DEPTH, (h + 1) * DEPTH)
                keep = before_keep[d, :, lanes]
                early = landed[k, d, h].astype(F32)
                before[d, h] = keep * early[:DEPTH] + before[d, h]
                before_keep[d, :, lanes] = keep * early[DEPTH : DEPTH + 1]

        @pl.when(exists)
        def _():
            scan_copy(k, d, stride, sent, landed, p_send, p_recv).wait_send()


def scan_states(state, offset, sent, landed, before, before_keep, p_send, p_recv):
    before[...] = jnp.zeros_like(before)
    before_keep[...] = jnp.ones_like(before_keep)
    for k in range(len(strides())):
        scan_start(k, state, offset, sent, landed, before, before_keep, p_send, p_recv)
        scan_close(k, state, sent, landed, before, before_keep, p_send, p_recv)


def local_kernel(
    query_pre, forget_fwd, forget_bwd, value, gap, added, initial, pool_in,
    out, carried_fwd, carried_bwd, entering, padded,
    state, offset, chunk_state, chunk_keep, sent, landed, before, before_keep, edge,
    p_send, p_recv, e_send, e_recv,
):
    length, width = query_pre.shape
    heads = width // DEPTH
    count = length // CHUNK
    row = lax.broadcasted_iota(jnp.int32, (CHUNK, CHUNK), 0)
    col = lax.broadcasted_iota(jnp.int32, (CHUNK, CHUNK), 1)
    lower = row >= col
    upper = row <= col
    lower_f, upper_f = lower.astype(F32), upper.astype(F32)
    lower_2 = jnp.concatenate([lower_f, lower_f], axis=1).astype(BF16)
    upper_2 = jnp.concatenate([upper_f, upper_f], axis=1).astype(BF16)
    exact = lax.Precision.HIGHEST

    def gates(pre, gap_row, sums):
        enter = gap_row * (1.0 / (1.0 + jnp.exp(pre[...].astype(F32))))
        keep = jnp.log1p(-enter)
        high = keep.astype(BF16)
        low = (keep - high.astype(F32)).astype(BF16)
        return enter, dot(sums, jnp.concatenate([high, low], axis=0))

    meet()
    edges_start(pool_in, edge, e_send, e_recv)
    state[...] = jnp.zeros_like(state)
    offset[...] = jnp.zeros_like(offset)

    def ascend(c, _):
        at = pl.ds(pl.multiple_of(c * CHUNK, CHUNK), CHUNK)
        x = query_pre[at, :].astype(F32)
        query = x / (1.0 + jnp.exp(-x))
        values = value[at, :]
        enter_f, run_f = gates(forget_fwd.at[at], gap[0:1, :], lower_2)
        enter_b, run_b = gates(forget_bwd.at[at], gap[1:2, :], upper_2)
        add = added[at, :]
        col_f = jnp.dot(lower_f, add, precision=exact, preferred_element_type=F32)
        col_b = jnp.dot(upper_f, add, precision=exact, preferred_element_type=F32)
        row_f = t_dot(add, upper_f, exact)
        row_b = t_dot(add, lower_f, exact)
        close_f, close_b = run_f[CHUNK - 1 : CHUNK, :], run_b[0:1, :]
        q_f, q_b = query * jnp.exp(run_f), query * jnp.exp(run_b)
        e_f, e_b = (enter_f * jnp.exp(-run_f)).astype(BF16), (enter_b * jnp.exp(-run_b)).astype(BF16)
        last_f, last_b = enter_f * jnp.exp(close_f - run_f), enter_b * jnp.exp(close_b - run_b)
        for h in range(heads):
            lanes = slice(h * DEPTH, (h + 1) * DEPTH)
            a_col, b_col = col_f[:, h : h + 1], col_b[:, h : h + 1]
            a_row, b_row = row_f[h : h + 1, :], row_b[h : h + 1, :]
            a_end, b_end = a_col[CHUNK - 1 : CHUNK, :], b_col[0:1, :]
            fade_f = jnp.exp(jnp.where(lower, a_col - a_row, -1e30))
            fade_b = jnp.exp(jnp.where(upper, b_col - b_row, -1e30))
            v = values[:, lanes]
            weight = (
                dot_t(q_f[:, lanes].astype(BF16), e_f[:, lanes]) * fade_f
                + dot_t(q_b[:, lanes].astype(BF16), e_b[:, lanes]) * fade_b
            )
            y = dot(weight.astype(BF16), v)
            reach = q_f[:, lanes] * jnp.exp(a_col)
            y = y + dot_t(reach.astype(BF16), state[0, h].astype(BF16))
            out[at, lanes] = y
            carried_fwd[at, lanes] = (reach * jnp.exp(offset[0, :, lanes])).astype(BF16)
            carried_bwd[at, lanes] = (q_b[:, lanes] * jnp.exp(b_col)).astype(BF16)
            total_f = close_f[:, lanes] + a_end
            total_b = close_b[:, lanes] + b_end
            ends_f = (last_f[:, lanes] * jnp.exp(a_end - a_col)).astype(BF16)
            ends_b = (last_b[:, lanes] * jnp.exp(b_end - b_col)).astype(BF16)
            state[0, h] = jnp.exp(total_f) * state[0, h] + t_dot(v, ends_f)
            chunk_state[c, h] = t_dot(v, ends_b)
            chunk_keep[c, :, lanes] = total_b
            offset[0, :, lanes] = offset[0, :, lanes] + total_f
        return 0

    lax.fori_loop(0, count, ascend, 0)

    def descend(i, _):
        c = count - 1 - i
        at = pl.ds(pl.multiple_of(c * CHUNK, CHUNK), CHUNK)
        for h in range(heads):
            lanes = slice(h * DEPTH, (h + 1) * DEPTH)
            reach = carried_bwd[at, lanes]
            out[at, lanes] = out[at, lanes] + dot_t(reach, state[1, h].astype(BF16))
            carried_bwd[at, lanes] = (
                reach.astype(F32) * jnp.exp(offset[1, :, lanes])
            ).astype(BF16)
            total = chunk_keep[c, :, lanes]
            state[1, h] = jnp.exp(total) * state[1, h] + chunk_state[c, h]
            offset[1, :, lanes] = offset[1, :, lanes] + total
        return 0

    lax.fori_loop(0, count, descend, 0)
    scan_states(state, offset, sent, landed, before, before_keep, p_send, p_recv)
    for h in range(heads):
        lanes = slice(h * DEPTH, (h + 1) * DEPTH)
        for d in range(2):
            s = before_keep[d, :, lanes] * initial[d, h].T + before[d, h]
            entering[h, :, d * DEPTH : (d + 1) * DEPTH] = s.astype(BF16)
    rim = edge.shape[1]
    padded[rim : rim + length, :] = pool_in[...]
    edges_close(pool_in, edge, e_send, e_recv)
    padded[:rim, :] = edge[0]
    padded[rim + length :, :] = edge[1]


def local_pass(query_pre, forget_fwd, forget_bwd, value, gap, added, initial, pool_in, rim):
    length, width = query_pre.shape
    heads = width // DEPTH
    count = length // CHUNK
    steps = len(strides())
    flat = jax.ShapeDtypeStruct((length, width), BF16)
    return pl.pallas_call(
        local_kernel,
        out_shape=[
            jax.ShapeDtypeStruct((length, width), F32), flat, flat,
            jax.ShapeDtypeStruct((heads, DEPTH, 2 * DEPTH), BF16),
            jax.ShapeDtypeStruct((length + 2 * rim, pool_in.shape[1]), BF16),
        ],
        in_specs=[VM] * 8,
        out_specs=[VM] * 5,
        scratch_shapes=[
            pltpu.VMEM((2, heads, DEPTH, DEPTH), F32),
            pltpu.VMEM((2, 1, width), F32),
            pltpu.VMEM((count, heads, DEPTH, DEPTH), F32),
            pltpu.VMEM((count, 1, width), F32),
            pltpu.VMEM((steps, 2, heads, DEPTH + 16, DEPTH), BF16),
            pltpu.VMEM((steps, 2, heads, DEPTH + 16, DEPTH), BF16),
            pltpu.VMEM((2, heads, DEPTH, DEPTH), F32),
            pltpu.VMEM((2, 1, width), F32),
            pltpu.VMEM((2, rim, pool_in.shape[1]), BF16),
            pltpu.SemaphoreType.DMA((steps, 2)),
            pltpu.SemaphoreType.DMA((steps, 2)),
            pltpu.SemaphoreType.DMA((2,)),
            pltpu.SemaphoreType.DMA((2,)),
        ],
        compiler_params=pltpu.CompilerParams(
            collective_id=2, has_side_effects=True, vmem_limit_bytes=VMEM_LIMIT
        ),
        name="local",
    )(query_pre, forget_fwd, forget_bwd, value, gap, added, initial, pool_in)


def block_of(begin, rows, refs, scratch, places):
    (local, carried_fwd, carried_bwd, gate_pre, head_gain, padded, mix, pool_gain, w_recur, w_pool) = refs
    entering, = scratch
    rim, sequence, first_row, window = places
    width = local.shape[1]
    heads = width // DEPTH
    at = pl.ds(begin, rows)
    recur = []
    for h in range(heads):
        lanes = slice(h * DEPTH, (h + 1) * DEPTH)
        reach = jnp.concatenate([carried_fwd[at, lanes], carried_bwd[at, lanes]], axis=1)
        both = local[at, lanes] + dot_t(reach, entering[h])
        both = both * lax.rsqrt(jnp.mean(both * both, axis=1, keepdims=True) + EPSILON)
        gate = gate_pre[at, lanes].astype(F32)
        recur.append((both * head_gain[:, lanes] / (1.0 + jnp.exp(-gate))).astype(BF16))
    total = dot(jnp.concatenate(recur, axis=1), w_recur[...])
    span = rows + 2 * rim
    near = padded[pl.ds(begin, span), :]
    target = first_row + begin + lax.broadcasted_iota(jnp.int32, (rows, span), 0)
    source = first_row + begin - rim + lax.broadcasted_iota(jnp.int32, (rows, span), 1)
    low = target - window // 2
    inside = (source >= low) & (source < low + window) & (source >= 0) & (source < sequence)
    start = first_row + begin + lax.broadcasted_iota(jnp.int32, (rows, 1), 0) - window // 2
    number = jnp.minimum(start + window, sequence) - jnp.maximum(start, 0)
    sums = dot(inside.astype(F32).astype(BF16), near)
    mean = sums / number.astype(F32)
    diff = (mean - padded[pl.ds(begin + rim, rows), :].astype(F32)).astype(BF16)
    pooled = (dot(diff, mix[0]) * pool_gain[...]).astype(BF16)
    return total + dot(pooled, w_pool[...])


def finish_kernel(groups, rim, *refs):
    entering, shared, out = refs[0], refs[1:11], refs[11]
    (kept, given, taken, sent, landed, g_send, g_recv, x_send, x_recv) = refs[12:]
    me, sibling, across, opposite = peers()
    greet(sibling, across)
    length = shared[0].shape[0]
    share = length // 4
    rows = kept.shape[1]
    pieces = share // rows
    group = lax.axis_index("tp") * groups
    window = jnp.left_shift(jnp.int32(2), group)
    places = (rim, length * lax.axis_size("sp"), lax.axis_index("sp") * length, window)

    def beside(i):
        return pltpu.make_async_remote_copy(
            given.at[i], taken.at[i], g_send.at[i], g_recv.at[i],
            device_id={"tp": sibling}, device_id_type=MESH,
        )

    def crossing(i):
        return pltpu.make_async_remote_copy(
            sent.at[i], landed.at[i], x_send.at[i], x_recv.at[i],
            device_id={"tp": across}, device_id_type=MESH,
        )

    def partial(owner, p):
        begin = pl.multiple_of(owner * share + p * rows, rows)
        return block_of(begin, rows, shared, (entering,), places).astype(BF16)

    def away(p, _):
        given[p] = partial(opposite, p)
        beside(p).start()
        mine = partial(across, p)
        beside(p).wait_recv()
        sent[p] = (mine.astype(F32) + taken[p].astype(F32)).astype(BF16)
        crossing(p).start()
        return 0

    lax.fori_loop(0, pieces, away, 0)

    def home(p, _):
        given[pieces + p] = partial(sibling, p)
        beside(pieces + p).start()
        kept[p] = partial(me, p)
        return 0

    lax.fori_loop(0, pieces, home, 0)

    def close(p, _):
        beside(pieces + p).wait_recv()
        crossing(p).wait_recv()
        total = kept[p].astype(F32) + taken[pieces + p].astype(F32) + landed[p].astype(F32)
        out[pl.ds(pl.multiple_of(p * rows, rows), rows), :] = total.astype(BF16)
        return 0

    lax.fori_loop(0, pieces, close, 0)
    for i in range(pieces):
        crossing(i).wait_send()
    for i in range(2 * pieces):
        beside(i).wait_send()


def finish(entering, shared, rim):
    length = shared[0].shape[0]
    features = shared[-1].shape[1]
    share, rows = length // 4, 128
    pieces = share // rows
    return pl.pallas_call(
        functools.partial(finish_kernel, shared[6].shape[0], rim),
        out_shape=jax.ShapeDtypeStruct((share, features), BF16),
        in_specs=[VM] * 11,
        out_specs=VM,
        scratch_shapes=[
            pltpu.VMEM((pieces, rows, features), BF16),
            pltpu.VMEM((2 * pieces, rows, features), BF16),
            pltpu.VMEM((2 * pieces, rows, features), BF16),
            pltpu.VMEM((pieces, rows, features), BF16),
            pltpu.VMEM((pieces, rows, features), BF16),
            pltpu.SemaphoreType.DMA((2 * pieces,)),
            pltpu.SemaphoreType.DMA((2 * pieces,)),
            pltpu.SemaphoreType.DMA((pieces,)),
            pltpu.SemaphoreType.DMA((pieces,)),
        ],
        compiler_params=pltpu.CompilerParams(
            collective_id=1, has_side_effects=True, vmem_limit_bytes=VMEM_LIMIT
        ),
        name="finish",
    )(entering, *shared)


def shards(
    tokens, norm_gain, w_query, w_forget_fwd, w_forget_bwd, w_value, w_gate, w_pool_in,
    forget_gap, added_log_retention, initial_state, head_gain, pool_mix, pool_gain,
    w_out_recur, w_out_pool,
):
    weights = (w_query, w_forget_fwd, w_forget_bwd, w_value, w_gate, w_pool_in)
    query_pre, forget_fwd, forget_bwd, value, gate_pre, pool_in = project(
        tokens, norm_gain[None, :], weights
    )
    rim = 16
    local, carried_fwd, carried_bwd, entering, padded = local_pass(
        query_pre, forget_fwd, forget_bwd, value, forget_gap, added_log_retention,
        initial_state, pool_in, rim,
    )
    shared = (
        local, carried_fwd, carried_bwd, gate_pre, head_gain[None, :], padded,
        pool_mix, pool_gain[None, :], w_out_recur, w_out_pool,
    )
    return finish(entering, shared, rim)


def solution(mesh):
    in_specs = (
        P("sp", "tp"), P(), P(None, "tp"), P(None, "tp"), P(None, "tp"), P(None, "tp"),
        P(None, "tp"), P(None, "tp"), P(None, "tp"), P("sp", "tp"), P(None, "tp", None, None),
        P("tp"), P("tp", None, None), P("tp"), P("tp", None), P("tp", None),
    )
    out_specs = P(("sp", "tp"), None)
    return jax.shard_map(shards, mesh=mesh, in_specs=in_specs, out_specs=out_specs, check_vma=False)
```

```python
import functools

import jax
import jax.numpy as jnp
from jax import lax
from jax.experimental import pallas as pl
from jax.experimental.pallas import tpu as pltpu
from jax.sharding import PartitionSpec as P

DEPTH = 128
CHUNK = 128
EPSILON = 1e-06
MESH = pl.DeviceIdType.MESH
F32 = jnp.float32
BF16 = jnp.bfloat16
VMEM_LIMIT = 60 * 1024 * 1024
ANY = pl.BlockSpec(memory_space=pl.ANY)
VM = pl.BlockSpec(memory_space=pltpu.VMEM)


def dot(a, b):
    return jnp.dot(a, b, preferred_element_type=F32)


def dot_t(a, b):
    return lax.dot_general(a, b, (((1,), (1,)), ((), ())), preferred_element_type=F32)


def t_dot(a, b, precision=None):
    return lax.dot_general(
        a, b, (((0,), (0,)), ((), ())), preferred_element_type=F32, precision=precision
    )


def peers():
    me = lax.axis_index("tp")
    sibling = me + 1 - 2 * lax.rem(me, 2)
    across = lax.rem(me + 2, 4)
    return me, sibling, across, lax.rem(sibling + 2, 4)


def greet(*devices):
    barrier = pltpu.get_barrier_semaphore()
    for device in devices:
        pl.semaphore_signal(barrier, inc=1, device_id={"tp": device}, device_id_type=MESH)
    pl.semaphore_wait(barrier, len(devices))


def project_kernel(pieces, tokens, gain, *refs):
    weights, outs = refs[:6], refs[6:12]
    held, wide, acc, square, w_sem, sib_sem, x_send, x_recv, f_send, f_recv = refs[12:]
    me, sibling, across, opposite = peers()
    length, width = tokens.shape
    rows = length // pieces
    loads = [pltpu.make_async_copy(w, wide.at[i], w_sem.at[i]) for i, w in enumerate(weights)]
    for load in loads:
        load.start()
    greet(sibling, across)

    def crossing(i):
        at = pl.ds(i * rows, rows)
        return pltpu.make_async_remote_copy(
            tokens.at[at], held.at[1, at], x_send.at[i], x_recv.at[i],
            device_id={"tp": across}, device_id_type=MESH,
        )

    def relay(i):
        at = pl.ds(i * rows, rows)
        return pltpu.make_async_remote_copy(
            held.at[1, at], held.at[2, at], f_send.at[i], f_recv.at[i],
            device_id={"tp": sibling}, device_id_type=MESH,
        )

    beside = pltpu.make_async_remote_copy(
        tokens, held.at[0], sib_sem.at[0], sib_sem.at[1],
        device_id={"tp": sibling}, device_id_type=MESH,
    )
    for i in range(pieces):
        crossing(i).start()
    beside.start()

    def part(block, owner, at, first):
        columns = pl.ds(pl.multiple_of(owner * width, width), width)
        x = block.astype(F32)
        total = jnp.sum(x * x, axis=1, keepdims=True)
        normed = (x * gain[:, columns]).astype(BF16)
        square[at, :] = total if first else square[at, :] + total
        for j in range(6):
            y = dot(normed, wide[j, columns, :])
            acc[j, at, :] = y if first else acc[j, at, :] + y

    for load in loads:
        load.wait()

    def own(i, _):
        at = pl.ds(pl.multiple_of(i * rows, rows), rows)
        part(tokens[at, :], me, at, True)
        return 0

    lax.fori_loop(0, pieces, own, 0)
    beside.wait()

    def near(i, _):
        at = pl.ds(pl.multiple_of(i * rows, rows), rows)
        part(held[0, at, :], sibling, at, False)
        return 0

    lax.fori_loop(0, pieces, near, 0)
    features = width * 4

    def far(i, _):
        at = pl.ds(pl.multiple_of(i * rows, rows), rows)
        crossing(i).wait_recv()
        relay(i).start()
        part(held[1, at, :], across, at, False)
        relay(i).wait_recv()
        part(held[2, at, :], opposite, at, False)
        scale = lax.rsqrt(square[at, :] / features + EPSILON)
        for j in range(6):
            outs[j][at, :] = (acc[j, at, :] * scale).astype(BF16)
        return 0

    lax.fori_loop(0, pieces, far, 0)
    for i in range(pieces):
        crossing(i).wait_send()
        relay(i).wait_send()


def project(tokens, gain, weights):
    length, width = tokens.shape
    depth, columns = weights[0].shape
    pieces = 4
    return pl.pallas_call(
        functools.partial(project_kernel, pieces),
        out_shape=[jax.ShapeDtypeStruct((length, columns), BF16)] * 6,
        in_specs=[VM, VM] + [ANY] * 6,
        out_specs=[VM] * 6,
        scratch_shapes=[
            pltpu.VMEM((3, length, width), BF16),
            pltpu.VMEM((6, depth, columns), BF16),
            pltpu.VMEM((6, length, columns), F32),
            pltpu.VMEM((length, 1), F32),
            pltpu.SemaphoreType.DMA((6,)),
            pltpu.SemaphoreType.DMA((2,)),
            pltpu.SemaphoreType.DMA((pieces,)),
            pltpu.SemaphoreType.DMA((pieces,)),
            pltpu.SemaphoreType.DMA((pieces,)),
            pltpu.SemaphoreType.DMA((pieces,)),
        ],
        compiler_params=pltpu.CompilerParams(
            collective_id=0, has_side_effects=True, vmem_limit_bytes=VMEM_LIMIT
        ),
        name="project",
    )(tokens, gain, *weights)


def strides():
    count = lax.axis_size("sp")
    return [1 << k for k in range(count.bit_length()) if 1 << k < count]


def partner(d, stride):
    me, count = lax.axis_index("sp"), lax.axis_size("sp")
    above, below = me + stride < count, me >= stride
    return (above, me + stride, below) if d == 0 else (below, me - stride, above)


def meet():
    barrier = pltpu.get_barrier_semaphore()
    for stride in strides():
        for d in range(2):
            exists, target, _ = partner(d, stride)

            @pl.when(exists)
            def _():
                pl.semaphore_signal(
                    barrier, inc=1, device_id={"sp": target}, device_id_type=MESH
                )

    number = jnp.int32(0)
    for stride in strides():
        for d in range(2):
            exists, _, _ = partner(d, stride)
            number = number + jnp.where(exists, 1, 0)
    pl.semaphore_wait(barrier, number)


def edge_copy(d, pool_in, edge, e_send, e_recv):
    length, rim = pool_in.shape[0], edge.shape[1]
    _, target, _ = partner(d, 1)
    begin = length - rim if d == 0 else 0
    return pltpu.make_async_remote_copy(
        pool_in.at[pl.ds(begin, rim)], edge.at[d], e_send.at[d], e_recv.at[d],
        device_id={"sp": target}, device_id_type=MESH,
    )


def edges_start(pool_in, edge, e_send, e_recv):
    for d in range(2):
        exists, _, source = partner(d, 1)

        @pl.when(exists)
        def _():
            edge_copy(d, pool_in, edge, e_send, e_recv).start()

        @pl.when(jnp.logical_not(source))
        def _():
            edge[d] = jnp.zeros(edge.shape[1:], edge.dtype)


def edges_close(pool_in, edge, e_send, e_recv):
    for d in range(2):
        exists, _, source = partner(d, 1)

        @pl.when(source)
        def _():
            edge_copy(d, pool_in, edge, e_send, e_recv).wait_recv()

        @pl.when(exists)
        def _():
            edge_copy(d, pool_in, edge, e_send, e_recv).wait_send()


def scan_copy(k, d, stride, sent, landed, p_send, p_recv):
    _, target, _ = partner(d, stride)
    return pltpu.make_async_remote_copy(
        sent.at[k, d], landed.at[k, d], p_send.at[k, d], p_recv.at[k, d],
        device_id={"sp": target}, device_id_type=MESH,
    )


def scan_start(k, state, offset, sent, landed, before, before_keep, p_send, p_recv):
    stride, heads = strides()[k], state.shape[1]
    for d in range(2):
        exists, _, _ = partner(d, stride)

        @pl.when(exists)
        def _():
            for h in range(heads):
                lanes = slice(h * DEPTH, (h + 1) * DEPTH)
                keep = jnp.exp(offset[d, :, lanes])
                sent[k, d, h, :DEPTH, :] = (keep * before[d, h] + state[d, h]).astype(BF16)
                sent[k, d, h, DEPTH:, :] = jnp.broadcast_to(
                    keep * before_keep[d, :, lanes], (16, DEPTH)
                ).astype(BF16)
            scan_copy(k, d, stride, sent, landed, p_send, p_recv).start()


def scan_close(k, state, sent, landed, before, before_keep, p_send, p_recv):
    stride, heads = strides()[k], state.shape[1]
    for d in range(2):
        exists, _, source = partner(d, stride)

        @pl.when(source)
        def _():
            scan_copy(k, d, stride, sent, landed, p_send, p_recv).wait_recv()
            for h in range(heads):
                lanes = slice(h * DEPTH, (h + 1) * DEPTH)
                keep = before_keep[d, :, lanes]
                early = landed[k, d, h].astype(F32)
                before[d, h] = keep * early[:DEPTH] + before[d, h]
                before_keep[d, :, lanes] = keep * early[DEPTH : DEPTH + 1]

        @pl.when(exists)
        def _():
            scan_copy(k, d, stride, sent, landed, p_send, p_recv).wait_send()


def local_kernel(
    query_pre, forget_fwd, forget_bwd, value, gap, added, initial, pool_in,
    out, carried_fwd, carried_bwd, entering, padded,
    state, offset, chunk_state, chunk_keep, sent, landed, before, before_keep, edge,
    p_send, p_recv, e_send, e_recv, enters, runs, cols, starts, offsets,
):
    length, width = query_pre.shape
    heads = width // DEPTH
    count = length // CHUNK
    row = lax.broadcasted_iota(jnp.int32, (CHUNK, CHUNK), 0)
    col = lax.broadcasted_iota(jnp.int32, (CHUNK, CHUNK), 1)
    lower = row >= col
    upper = row <= col
    lower_f, upper_f = lower.astype(F32), upper.astype(F32)
    lower_2 = jnp.concatenate([lower_f, lower_f], axis=1).astype(BF16)
    upper_2 = jnp.concatenate([upper_f, upper_f], axis=1).astype(BF16)
    exact = lax.Precision.HIGHEST

    def gates(pre, gap_row, sums):
        enter = gap_row * (1.0 / (1.0 + jnp.exp(pre[...].astype(F32))))
        keep = jnp.log1p(-enter)
        high = keep.astype(BF16)
        low = (keep - high.astype(F32)).astype(BF16)
        return enter, dot(sums, jnp.concatenate([high, low], axis=0))

    meet()
    edges_start(pool_in, edge, e_send, e_recv)
    state[...] = jnp.zeros_like(state)
    offset[...] = jnp.zeros_like(offset)

    def ascend(c, _):
        at = pl.ds(pl.multiple_of(c * CHUNK, CHUNK), CHUNK)
        values = value[at, :]
        enter_f, run_f = gates(forget_fwd.at[at], gap[0:1, :], lower_2)
        enter_b, run_b = gates(forget_bwd.at[at], gap[1:2, :], upper_2)
        add = added[at, :]
        col_f = jnp.dot(lower_f, add, precision=exact, preferred_element_type=F32)
        col_b = jnp.dot(upper_f, add, precision=exact, preferred_element_type=F32)
        enters[0, at, :], enters[1, at, :] = enter_f, enter_b
        runs[0, at, :], runs[1, at, :] = run_f, run_b
        cols[0, at, :], cols[1, at, :] = col_f, col_b
        close_f, close_b = run_f[CHUNK - 1 : CHUNK, :], run_b[0:1, :]
        last_f, last_b = enter_f * jnp.exp(close_f - run_f), enter_b * jnp.exp(close_b - run_b)
        offsets[0, c] = offset[0]
        for h in range(heads):
            lanes = slice(h * DEPTH, (h + 1) * DEPTH)
            a_col, b_col = col_f[:, h : h + 1], col_b[:, h : h + 1]
            a_end, b_end = a_col[CHUNK - 1 : CHUNK, :], b_col[0:1, :]
            v = values[:, lanes]
            total_f = close_f[:, lanes] + a_end
            ends_f = (last_f[:, lanes] * jnp.exp(a_end - a_col)).astype(BF16)
            ends_b = (last_b[:, lanes] * jnp.exp(b_end - b_col)).astype(BF16)
            ends = t_dot(v, jnp.concatenate([ends_f, ends_b], axis=1))
            starts[c, h, :, :DEPTH] = state[0, h].astype(BF16)
            state[0, h] = jnp.exp(total_f) * state[0, h] + ends[:, :DEPTH]
            chunk_state[c, h] = ends[:, DEPTH:]
            chunk_keep[c, :, lanes] = close_b[:, lanes] + b_end
            offset[0, :, lanes] = offset[0, :, lanes] + total_f
        return 0

    lax.fori_loop(0, count, ascend, 0)

    def descend(i, _):
        c = count - 1 - i
        offsets[1, c] = offset[1]
        for h in range(heads):
            lanes = slice(h * DEPTH, (h + 1) * DEPTH)
            starts[c, h, :, DEPTH:] = state[1, h].astype(BF16)
            total = chunk_keep[c, :, lanes]
            state[1, h] = jnp.exp(total) * state[1, h] + chunk_state[c, h]
            offset[1, :, lanes] = offset[1, :, lanes] + total
        return 0

    lax.fori_loop(0, count, descend, 0)

    def output(c, _):
        at = pl.ds(pl.multiple_of(c * CHUNK, CHUNK), CHUNK)
        x = query_pre[at, :].astype(F32)
        query = x / (1.0 + jnp.exp(-x))
        values = value[at, :]
        run_f, run_b = runs[0, at, :], runs[1, at, :]
        col_f, col_b = cols[0, at, :], cols[1, at, :]
        add = added[at, :]
        row_f = t_dot(add, upper_f, exact)
        row_b = t_dot(add, lower_f, exact)
        q_f, q_b = query * jnp.exp(run_f), query * jnp.exp(run_b)
        e_f = (enters[0, at, :] * jnp.exp(-run_f)).astype(BF16)
        e_b = (enters[1, at, :] * jnp.exp(-run_b)).astype(BF16)
        for h in range(heads):
            lanes = slice(h * DEPTH, (h + 1) * DEPTH)
            a_col, b_col = col_f[:, h : h + 1], col_b[:, h : h + 1]
            fade_f = jnp.exp(jnp.where(lower, a_col - row_f[h : h + 1, :], -1e30))
            fade_b = jnp.exp(jnp.where(upper, b_col - row_b[h : h + 1, :], -1e30))
            weight = (
                dot_t(q_f[:, lanes].astype(BF16), e_f[:, lanes]) * fade_f
                + dot_t(q_b[:, lanes].astype(BF16), e_b[:, lanes]) * fade_b
            )
            reach_f = q_f[:, lanes] * jnp.exp(a_col)
            reach_b = q_b[:, lanes] * jnp.exp(b_col)
            reach = jnp.concatenate([reach_f, reach_b], axis=1).astype(BF16)
            out[at, lanes] = dot(weight.astype(BF16), values[:, lanes]) + dot_t(reach, starts[c, h])
            carried_fwd[at, lanes] = (reach_f * jnp.exp(offsets[0, c, :, lanes])).astype(BF16)
            carried_bwd[at, lanes] = (reach_b * jnp.exp(offsets[1, c, :, lanes])).astype(BF16)
        return 0

    before[...] = jnp.zeros_like(before)
    before_keep[...] = jnp.ones_like(before_keep)
    steps = len(strides())
    for k in range(steps):
        scan_start(k, state, offset, sent, landed, before, before_keep, p_send, p_recv)
        lax.fori_loop(k * count // steps, (k + 1) * count // steps, output, 0)
        scan_close(k, state, sent, landed, before, before_keep, p_send, p_recv)
    for h in range(heads):
        lanes = slice(h * DEPTH, (h + 1) * DEPTH)
        for d in range(2):
            s = before_keep[d, :, lanes] * initial[d, h].T + before[d, h]
            entering[h, :, d * DEPTH : (d + 1) * DEPTH] = s.astype(BF16)
    rim = edge.shape[1]
    padded[rim : rim + length, :] = pool_in[...]
    edges_close(pool_in, edge, e_send, e_recv)
    padded[:rim, :] = edge[0]
    padded[rim + length :, :] = edge[1]


def local_pass(query_pre, forget_fwd, forget_bwd, value, gap, added, initial, pool_in, rim):
    length, width = query_pre.shape
    heads = width // DEPTH
    count = length // CHUNK
    steps = len(strides())
    flat = jax.ShapeDtypeStruct((length, width), BF16)
    return pl.pallas_call(
        local_kernel,
        out_shape=[
            jax.ShapeDtypeStruct((length, width), F32), flat, flat,
            jax.ShapeDtypeStruct((heads, DEPTH, 2 * DEPTH), BF16),
            jax.ShapeDtypeStruct((length + 2 * rim, pool_in.shape[1]), BF16),
        ],
        in_specs=[VM] * 8,
        out_specs=[VM] * 5,
        scratch_shapes=[
            pltpu.VMEM((2, heads, DEPTH, DEPTH), F32),
            pltpu.VMEM((2, 1, width), F32),
            pltpu.VMEM((count, heads, DEPTH, DEPTH), F32),
            pltpu.VMEM((count, 1, width), F32),
            pltpu.VMEM((steps, 2, heads, DEPTH + 16, DEPTH), BF16),
            pltpu.VMEM((steps, 2, heads, DEPTH + 16, DEPTH), BF16),
            pltpu.VMEM((2, heads, DEPTH, DEPTH), F32),
            pltpu.VMEM((2, 1, width), F32),
            pltpu.VMEM((2, rim, pool_in.shape[1]), BF16),
            pltpu.SemaphoreType.DMA((steps, 2)),
            pltpu.SemaphoreType.DMA((steps, 2)),
            pltpu.SemaphoreType.DMA((2,)),
            pltpu.SemaphoreType.DMA((2,)),
            pltpu.VMEM((2, length, width), F32),
            pltpu.VMEM((2, length, width), F32),
            pltpu.VMEM((2, length, heads), F32),
            pltpu.VMEM((count, heads, DEPTH, 2 * DEPTH), BF16),
            pltpu.VMEM((2, count, 1, width), F32),
        ],
        compiler_params=pltpu.CompilerParams(
            collective_id=2, has_side_effects=True, vmem_limit_bytes=VMEM_LIMIT
        ),
        name="local",
    )(query_pre, forget_fwd, forget_bwd, value, gap, added, initial, pool_in)


def block_of(begin, rows, refs, scratch, places):
    (local, carried_fwd, carried_bwd, gate_pre, head_gain, padded, mix, pool_gain, w_recur, w_pool) = refs
    entering, = scratch
    rim, sequence, first_row, window = places
    width = local.shape[1]
    heads = width // DEPTH
    at = pl.ds(begin, rows)
    recur = []
    for h in range(heads):
        lanes = slice(h * DEPTH, (h + 1) * DEPTH)
        reach = jnp.concatenate([carried_fwd[at, lanes], carried_bwd[at, lanes]], axis=1)
        both = local[at, lanes] + dot_t(reach, entering[h])
        both = both * lax.rsqrt(jnp.mean(both * both, axis=1, keepdims=True) + EPSILON)
        gate = gate_pre[at, lanes].astype(F32)
        recur.append((both * head_gain[:, lanes] / (1.0 + jnp.exp(-gate))).astype(BF16))
    total = dot(jnp.concatenate(recur, axis=1), w_recur[...])
    span = rows + 2 * rim
    near = padded[pl.ds(begin, span), :]
    target = first_row + begin + lax.broadcasted_iota(jnp.int32, (rows, span), 0)
    source = first_row + begin - rim + lax.broadcasted_iota(jnp.int32, (rows, span), 1)
    low = target - window // 2
    inside = (source >= low) & (source < low + window) & (source >= 0) & (source < sequence)
    start = first_row + begin + lax.broadcasted_iota(jnp.int32, (rows, 1), 0) - window // 2
    number = jnp.minimum(start + window, sequence) - jnp.maximum(start, 0)
    sums = dot(inside.astype(F32).astype(BF16), near)
    mean = sums / number.astype(F32)
    diff = (mean - padded[pl.ds(begin + rim, rows), :].astype(F32)).astype(BF16)
    pooled = (dot(diff, mix[0]) * pool_gain[...]).astype(BF16)
    return total + dot(pooled, w_pool[...])


def finish_kernel(groups, rim, *refs):
    entering, shared, out = refs[0], refs[1:11], refs[11]
    (kept, given, taken, sent, landed, g_send, g_recv, x_send, x_recv) = refs[12:]
    me, sibling, across, opposite = peers()
    greet(sibling, across)
    length = shared[0].shape[0]
    share = length // 4
    rows = kept.shape[1]
    pieces = share // rows
    group = lax.axis_index("tp") * groups
    window = jnp.left_shift(jnp.int32(2), group)
    places = (rim, length * lax.axis_size("sp"), lax.axis_index("sp") * length, window)

    def beside(i):
        return pltpu.make_async_remote_copy(
            given.at[i], taken.at[i], g_send.at[i], g_recv.at[i],
            device_id={"tp": sibling}, device_id_type=MESH,
        )

    def crossing(i):
        return pltpu.make_async_remote_copy(
            sent.at[i], landed.at[i], x_send.at[i], x_recv.at[i],
            device_id={"tp": across}, device_id_type=MESH,
        )

    def partial(owner, p):
        begin = pl.multiple_of(owner * share + p * rows, rows)
        return block_of(begin, rows, shared, (entering,), places).astype(BF16)

    def away(p, _):
        given[p] = partial(opposite, p)
        beside(p).start()
        mine = partial(across, p)
        beside(p).wait_recv()
        sent[p] = (mine.astype(F32) + taken[p].astype(F32)).astype(BF16)
        crossing(p).start()
        return 0

    lax.fori_loop(0, pieces, away, 0)

    def home(p, _):
        given[pieces + p] = partial(sibling, p)
        beside(pieces + p).start()
        kept[p] = partial(me, p)
        return 0

    lax.fori_loop(0, pieces, home, 0)

    def close(p, _):
        beside(pieces + p).wait_recv()
        crossing(p).wait_recv()
        total = kept[p].astype(F32) + taken[pieces + p].astype(F32) + landed[p].astype(F32)
        out[pl.ds(pl.multiple_of(p * rows, rows), rows), :] = total.astype(BF16)
        return 0

    lax.fori_loop(0, pieces, close, 0)
    for i in range(pieces):
        crossing(i).wait_send()
    for i in range(2 * pieces):
        beside(i).wait_send()


def finish(entering, shared, rim):
    length = shared[0].shape[0]
    features = shared[-1].shape[1]
    share, rows = length // 4, 128
    pieces = share // rows
    return pl.pallas_call(
        functools.partial(finish_kernel, shared[6].shape[0], rim),
        out_shape=jax.ShapeDtypeStruct((share, features), BF16),
        in_specs=[VM] * 11,
        out_specs=VM,
        scratch_shapes=[
            pltpu.VMEM((pieces, rows, features), BF16),
            pltpu.VMEM((2 * pieces, rows, features), BF16),
            pltpu.VMEM((2 * pieces, rows, features), BF16),
            pltpu.VMEM((pieces, rows, features), BF16),
            pltpu.VMEM((pieces, rows, features), BF16),
            pltpu.SemaphoreType.DMA((2 * pieces,)),
            pltpu.SemaphoreType.DMA((2 * pieces,)),
            pltpu.SemaphoreType.DMA((pieces,)),
            pltpu.SemaphoreType.DMA((pieces,)),
        ],
        compiler_params=pltpu.CompilerParams(
            collective_id=1, has_side_effects=True, vmem_limit_bytes=VMEM_LIMIT
        ),
        name="finish",
    )(entering, *shared)


def shards(
    tokens, norm_gain, w_query, w_forget_fwd, w_forget_bwd, w_value, w_gate, w_pool_in,
    forget_gap, added_log_retention, initial_state, head_gain, pool_mix, pool_gain,
    w_out_recur, w_out_pool,
):
    weights = (w_query, w_forget_fwd, w_forget_bwd, w_value, w_gate, w_pool_in)
    query_pre, forget_fwd, forget_bwd, value, gate_pre, pool_in = project(
        tokens, norm_gain[None, :], weights
    )
    rim = 16
    local, carried_fwd, carried_bwd, entering, padded = local_pass(
        query_pre, forget_fwd, forget_bwd, value, forget_gap, added_log_retention,
        initial_state, pool_in, rim,
    )
    shared = (
        local, carried_fwd, carried_bwd, gate_pre, head_gain[None, :], padded,
        pool_mix, pool_gain[None, :], w_out_recur, w_out_pool,
    )
    return finish(entering, shared, rim)


def solution(mesh):
    in_specs = (
        P("sp", "tp"), P(), P(None, "tp"), P(None, "tp"), P(None, "tp"), P(None, "tp"),
        P(None, "tp"), P(None, "tp"), P(None, "tp"), P("sp", "tp"), P(None, "tp", None, None),
        P("tp"), P("tp", None, None), P("tp"), P("tp", None), P("tp", None),
    )
    out_specs = P(("sp", "tp"), None)
    return jax.shard_map(shards, mesh=mesh, in_specs=in_specs, out_specs=out_specs, check_vma=False)
```
